32 devices in a mesh: ep: 16 (over z, y, x), tp: 2 (over core).
Axes of the slice: x: 2, y: 2, z: 4, core: 2. Of those that a mesh axis runs over, the one named last changes fastest.
Arguments:
- tokens: bfloat16 [2048, 2048], P('ep'), may hold values from -6 to 6
- cotangent: bfloat16 [2048, 2048], P('ep'), may hold values from -0.625 to 0.625
- routes: int32 [2048, 2], P('ep'), may hold values from 0 to 15, as said below
- router_group: bfloat16 [2048, 4], replicated, may hold values from -0.125 to 0.125
- router_expert: bfloat16 [2048, 16], replicated, may hold values from -0.125 to 0.125
- gate_proj: bfloat16 [16, 2048, 512], P('ep', None, 'tp'), may hold values from -0.125 to 0.125
- up_proj: bfloat16 [16, 2048, 512], P('ep', None, 'tp'), may hold values from -0.125 to 0.125
- down_proj: bfloat16 [16, 512, 2048], P('ep', 'tp'), may hold values from -0.25 to 0.25
Outputs:
- token_grad: bfloat16 [2048, 2048], P('ep', 'tp')
- gate_grad: bfloat16 [16, 2048, 512], P('ep', None, 'tp')
- up_grad: bfloat16 [16, 2048, 512], P('ep', None, 'tp')
- down_grad: bfloat16 [16, 512, 2048], P('ep', 'tp')
- gate_rows: float32 [16, 2048], P('ep')
- up_rows: float32 [16, 2048], P('ep')
- down_rows: float32 [16, 512], P('ep', 'tp')
- router_expert_grad: float32 [2048, 16], P(('ep', 'tp'))
- router_group_grad: float32 [2048, 4], P(('ep', 'tp'))
- router_rows: float32 [2048], P(('ep', 'tp'))
The draws below stay inside these ranges and needn't reach their ends.
Inputs may be any that keep to these rules, and one draw needn't show every extreme that they name: `routes`: the 2 entries of a row are different experts of one group: their quotients by 4 are equal. Among the rows of one device no expert is named more than 32 times, and the experts of one group, the same for all devices, are each named exactly 32 times by the rows of every device.
All inputs are finite; a program needn't handle non-finite values.
Results may differ from the reference program's by a relative error of at most 0.014.
Values may be sent and summed in bfloat16 or wider, within the bound.
A program may use at most 64 MiB of HBM per device.

```python
import jax
import jax.numpy as jnp
from jax import lax

D = 2048
FF = 512
TOK_DEV = 128
GROUPS = 4
TOP = 2
EXPERTS = 16
GROUP_SIZE = 4
TOKENS = 2048
N_TP = 2


def draw_routes(key, part):
    blocks = TOKENS // TOK_DEV
    half_rows = TOK_DEV // 2
    others_rows = TOK_DEV - half_rows
    favored = jax.random.randint(jax.random.fold_in(key, 11), (), 0, GROUPS)
    group_ids = jnp.arange(GROUPS, dtype=jnp.int32)
    is_favored = group_ids[None, :] == favored
    shares = jax.random.randint(jax.random.fold_in(key, 12), (blocks, GROUPS), 2, 5)
    shares = jnp.where(is_favored, 0, shares)
    base_rows = others_rows * shares // jnp.sum(shares, axis=1, keepdims=True)
    leftover = others_rows - jnp.sum(base_rows, axis=1, keepdims=True)
    other_rank = jnp.cumsum(jnp.where(is_favored, 0, 1), axis=1) - 1
    extra_rows = jnp.where(jnp.logical_and(jnp.logical_not(is_favored), other_rank < leftover), 1, 0)
    counts = base_rows + extra_rows + jnp.where(is_favored, half_rows, 0)
    group_end = jnp.cumsum(counts, axis=1)
    group_start = group_end - counts
    position = jnp.arange(TOK_DEV, dtype=jnp.int32)
    labels = jnp.sum((group_end[:, None, :] <= position[None, :, None]).astype(jnp.int32), axis=2)
    within = position[None, :] - jnp.take_along_axis(group_start, labels, axis=1)
    rotate = jax.random.randint(jax.random.fold_in(key, 13), (blocks, GROUPS), 0, GROUP_SIZE)
    offset = jax.random.randint(jax.random.fold_in(key, 14), (blocks, GROUPS), 0, GROUP_SIZE - 1)
    first_pick = (within + jnp.take_along_axis(rotate, labels, axis=1)) % GROUP_SIZE
    turned = (jnp.take_along_axis(offset, labels, axis=1) + within // GROUP_SIZE) % (GROUP_SIZE - 1)
    second_pick = (first_pick + 1 + turned) % GROUP_SIZE
    chosen = jnp.stack([labels * GROUP_SIZE + first_pick, labels * GROUP_SIZE + second_pick], axis=2)
    block_keys = jax.random.split(jax.random.fold_in(key, 15), blocks)
    shuffles = jax.vmap(lambda subkey: jax.random.permutation(subkey, TOK_DEV))(block_keys)
    chosen = jnp.take_along_axis(chosen, shuffles[:, :, None], axis=1)
    return chosen.reshape(TOKENS, TOP).astype(jnp.int32)


def spiked(values, rng, source, target, blocks, factor):
    def block_of(axis_at):
        return (jnp.arange(values.shape[axis_at]) // (values.shape[axis_at] // blocks)).reshape((-1,) + (1,) * (values.ndim - 1 - axis_at))

    first = jax.random.permutation(rng, blocks)[block_of(target)]
    other_side = (block_of(target) + blocks // 2) % blocks
    return jnp.where((block_of(source) == first) | (block_of(source) == other_side), factor * values, values)


def level_of(key, shape, cuts, low, high):
    def one(dim, shards_of):
        heights = jax.random.uniform(jax.random.fold_in(jax.random.fold_in(key, 6), dim), (shards_of,), jnp.float32, low / len(cuts), high / len(cuts))
        return jnp.repeat(jnp.exp(heights), shape[dim] // shards_of).reshape((-1,) + (1,) * (len(shape) - dim - 1))

    factor_of = one(*cuts[0])
    for cut in cuts[1:]:
        factor_of = factor_of * one(*cut)
    return factor_of


def noise(key, shape, width, most, pieces=(), kind=jnp.bfloat16):
    loudness = level_of(key, shape, pieces, -0.22, 0.18) if pieces else 1.0
    result = jax.random.normal(key, shape, jnp.float32) * width * loudness
    return jnp.minimum(jnp.maximum(result, -most), most).astype(kind)


def heavy_noise(rng, extent, width, reach, pieces, heavy, kind=jnp.bfloat16):
    array = width * jax.random.normal(rng, extent, jnp.float32)
    if pieces:
        array = array * level_of(rng, extent, pieces, -0.22, 0.18)
    return jnp.clip(spiked(array, jax.random.fold_in(rng, 3), *heavy), -reach, reach).astype(kind)


def setup_inputs(seed: int = 0) -> dict:
    keys = jax.random.split(jax.random.key(seed), 9)
    tokens = heavy_noise(keys[0], (TOKENS, D), 1.0, 6.0, ((0, 16),), (0, 1, 16, 2.0))
    cotangent = noise(keys[1], (TOKENS, D), 0.1, 0.625, ((0, 16),))
    routes = draw_routes(jax.random.fold_in(keys[8], 71), 0)
    router_group = noise(keys[3], (D, GROUPS), D ** -0.5, 0.125)
    router_expert = noise(keys[4], (D, EXPERTS), D ** -0.5, 0.125)
    gate_proj = noise(keys[5], (EXPERTS, D, FF), D ** -0.5, 0.125, ((0, 16), (2, 2)))
    up_proj = noise(keys[6], (EXPERTS, D, FF), D ** -0.5, 0.125, ((0, 16), (2, 2)))
    down_proj = noise(keys[7], (EXPERTS, FF, D), FF ** -0.5, 0.25, ((0, 16), (1, 2)))
    return dict(tokens=tokens, cotangent=cotangent, routes=routes, router_group=router_group, router_expert=router_expert, gate_proj=gate_proj, up_proj=up_proj, down_proj=down_proj)


tile_rows = 128


def contract_rows(left_side, right_side):
    return lax.dot_general(left_side, right_side, (((0,), (0,)), ((), ())), preferred_element_type=jnp.float32)


def contract_cols(left_side, right_side):
    return lax.dot_general(left_side, right_side, (((1,), (1,)), ((), ())), preferred_element_type=jnp.float32)


def router_forward(tokens, routes, router_group, router_expert):
    groups = router_group.shape[1]
    experts = router_expert.shape[1]
    group_logits = jnp.dot(tokens, router_group, preferred_element_type=jnp.float32)
    expert_logits = jnp.dot(tokens, router_expert, preferred_element_type=jnp.float32)
    group_exp = jnp.exp(group_logits)
    group_prob = group_exp / jnp.sum(group_exp, axis=1, keepdims=True)
    chosen_group = routes[:, 0] // (experts // groups)
    group_onehot = (chosen_group[:, None] == jnp.arange(groups, dtype=jnp.int32)[None, :]).astype(jnp.float32)
    picked = jnp.sum(group_prob * group_onehot, axis=1)
    chosen_logits = jnp.take_along_axis(expert_logits, routes, axis=1)
    paired_exp = jnp.exp(chosen_logits)
    paired = paired_exp / jnp.sum(paired_exp, axis=1, keepdims=True)
    return group_prob, group_onehot, picked, paired


def router_backward(dweight, routes, group_prob, group_onehot, picked, paired, experts):
    dpicked = jnp.sum(dweight * paired, axis=1)
    dpaired = dweight * picked[:, None]
    dchosen = paired * (dpaired - jnp.sum(paired * dpaired, axis=1, keepdims=True))
    dgroup = ((dpicked * picked)[:, None] * (group_onehot - group_prob)).astype(jnp.bfloat16)
    expert_onehot = (routes[:, :, None] == jnp.arange(experts, dtype=jnp.int32)[None, None, :]).astype(jnp.float32)
    dexpert = jnp.sum(dchosen[:, :, None] * expert_onehot, axis=1).astype(jnp.bfloat16)
    return dgroup, dexpert


def reference(tokens, cotangent, routes, router_group, router_expert, gate_proj, up_proj, down_proj):
    group_prob, group_onehot, picked, paired = router_forward(tokens, routes, router_group, router_expert)
    weights = (picked[:, None] * paired).astype(jnp.bfloat16)
    assigned = TOKENS * TOP
    flat_ids = routes.reshape(assigned).astype(jnp.int32)
    counts = jnp.zeros((EXPERTS,), jnp.int32).at[flat_ids].add(1)
    tile_count = ((counts + (tile_rows - 1)) // tile_rows).astype(jnp.int32)
    tile_end = jnp.cumsum(tile_count).astype(jnp.int32)
    tile_begin = (tile_end - tile_count).astype(jnp.int32)
    count_begin = (jnp.cumsum(counts).astype(jnp.int32) - counts).astype(jnp.int32)
    ordering = jnp.argsort(flat_ids, stable=True).astype(jnp.int32)
    sorted_ids = flat_ids[ordering]
    ranking = jnp.arange(assigned, dtype=jnp.int32) - count_begin[sorted_ids]
    padded_pos = (tile_begin[sorted_ids] * tile_rows + ranking).astype(jnp.int32)
    tile_total = (assigned + tile_rows - 1) // tile_rows + EXPERTS
    owners = jnp.full((tile_total * tile_rows,), assigned, jnp.int32).at[padded_pos].set(ordering)
    tile_marks = jnp.arange(tile_total, dtype=jnp.int32)[:, None]
    tile_expert = jnp.minimum(jnp.sum((tile_end[None, :] <= tile_marks).astype(jnp.int32), axis=1), EXPERTS - 1).astype(jnp.int32)
    flat_weights = weights.reshape(assigned)
    piece_width = FF // N_TP

    def tile_step(totals, tile_index):
        grad_gate, grad_up, grad_down = totals
        expert = tile_expert[tile_index]
        members = lax.dynamic_slice_in_dim(owners, tile_index * tile_rows, tile_rows)
        source_rows = members // TOP
        inputs = jnp.take(tokens, source_rows, axis=0, mode="fill", fill_value=0)
        upstream = jnp.take(cotangent, source_rows, axis=0, mode="fill", fill_value=0)
        slot_scale = jnp.take(flat_weights, members, axis=0, mode="fill", fill_value=0).astype(jnp.float32)
        gate_mat = gate_proj[expert]
        up_mat = up_proj[expert]
        down_mat = down_proj[expert]
        gate_pre = jnp.dot(inputs, gate_mat, preferred_element_type=jnp.float32)
        up_pre = jnp.dot(inputs, up_mat, preferred_element_type=jnp.float32)
        sigmoid_gate = jax.nn.sigmoid(gate_pre)
        hidden = (gate_pre * sigmoid_gate * up_pre).astype(jnp.bfloat16)
        pulled = contract_cols(upstream, down_mat)
        weight_part = jnp.sum(pulled * hidden.astype(jnp.float32), axis=1)
        dhidden = slot_scale[:, None] * pulled
        gate_delta = (dhidden * up_pre * sigmoid_gate * (1.0 + gate_pre * (1.0 - sigmoid_gate))).astype(jnp.bfloat16)
        up_delta = (dhidden * gate_pre * sigmoid_gate).astype(jnp.bfloat16)
        scaled_cot = (slot_scale[:, None] * upstream.astype(jnp.float32)).astype(jnp.bfloat16)
        grad_gate = grad_gate.at[expert].add(contract_rows(inputs, gate_delta))
        grad_up = grad_up.at[expert].add(contract_rows(inputs, up_delta))
        grad_down = grad_down.at[expert].add(contract_rows(hidden, scaled_cot))
        token_total = jnp.zeros((tile_rows, D), jnp.float32)
        for piece_index in range(N_TP):
            first_col = piece_index * piece_width
            last_col = first_col + piece_width
            piece_term = contract_cols(gate_delta[:, first_col:last_col], gate_mat[:, first_col:last_col])
            piece_term = piece_term + contract_cols(up_delta[:, first_col:last_col], up_mat[:, first_col:last_col])
            token_total = token_total + piece_term.astype(jnp.bfloat16).astype(jnp.float32)
        return (grad_gate, grad_up, grad_down), (token_total.astype(jnp.bfloat16), weight_part)

    start_totals = (jnp.zeros((EXPERTS, D, FF), jnp.float32), jnp.zeros((EXPERTS, D, FF), jnp.float32),
                    jnp.zeros((EXPERTS, FF, D), jnp.float32))
    totals, tile_outputs = lax.scan(tile_step, start_totals, jnp.arange(tile_total, dtype=jnp.int32))
    grad_gate, grad_up, grad_down = totals
    token_tiles, weight_tiles = tile_outputs
    position = jnp.zeros((assigned,), jnp.int32).at[ordering].set(padded_pos)
    token_rows = token_tiles.reshape(tile_total * tile_rows, D)[position]
    expert_part = jnp.sum(token_rows.reshape(TOKENS, TOP, D).astype(jnp.float32), axis=1)
    dweight = weight_tiles.reshape(tile_total * tile_rows)[position].astype(jnp.bfloat16).astype(jnp.float32)
    dweight = dweight.reshape(TOKENS, TOP)
    dgroup, dexpert = router_backward(dweight, routes, group_prob, group_onehot, picked, paired, EXPERTS)
    router_part = contract_cols(dgroup, router_group) + contract_cols(dexpert, router_expert)
    token_grad = (expert_part + router_part).astype(jnp.bfloat16)
    router_expert_grad = contract_rows(tokens, dexpert)
    router_group_grad = contract_rows(tokens, dgroup)
    router_rows = jnp.sum(router_expert_grad * router_expert_grad, axis=1) + jnp.sum(router_group_grad * router_group_grad, axis=1)
    gate_rows = jnp.sum(grad_gate * grad_gate, axis=2)
    up_rows = jnp.sum(grad_up * grad_up, axis=2)
    down_rows = jnp.sum(grad_down * grad_down, axis=2)
    return (token_grad, grad_gate.astype(jnp.bfloat16), grad_up.astype(jnp.bfloat16), grad_down.astype(jnp.bfloat16),
            gate_rows, up_rows, down_rows, router_expert_grad, router_group_grad, router_rows)
```

```python
import functools

import jax
import jax.numpy as jnp
from jax import lax
from jax.experimental import pallas as pl
from jax.experimental.pallas import tpu as pltpu
from jax.sharding import PartitionSpec as P

MESH = pl.DeviceIdType.MESH
BF = jnp.bfloat16
F32 = jnp.float32
TINY = 2.0**-126


def mm(a, b, da=1, db=0):
    return lax.dot_general(a, b, (((da,), (db,)), ((), ())), preferred_element_type=F32)


def lanes_of(shape, dim=1):
    return lax.broadcasted_iota(jnp.int32, shape, dim)


class Sizes:
    pass


def sizes_of(mesh, tokens, routes, router_group, router_expert, gate_proj):
    z = Sizes()
    z.n_ep, z.n_tp = mesh["ep"], mesh["tp"]
    z.rows, z.width = tokens.shape
    z.top = routes.shape[1]
    z.groups, z.experts = router_group.shape[1], router_expert.shape[1]
    z.gs = z.experts // z.groups
    z.cap = z.rows // z.gs
    z.gr = z.gs * z.cap // z.top
    z.r1 = z.groups * z.gr
    z.sl = z.groups * z.cap
    z.pairs = z.gs * z.sl
    z.ff = gate_proj.shape[2]
    z.cw = z.width // z.n_tp
    z.half_chunks = 2
    z.nc = 2 * z.half_chunks
    z.cc = z.cw // z.half_chunks
    z.rl = -(-(z.experts + z.groups) // 128) * 128
    z.rw = -(-(z.experts + z.groups) // 8) * 8
    z.ch = z.width // z.n_ep
    z.reduce_here = z.ch % 128 == 0 and z.n_ep % 2 == 0
    assert z.experts == z.n_ep and z.n_tp == 2 and z.top == 2
    assert z.sl & (z.sl - 1) == 0 and z.gr & (z.gr - 1) == 0
    return z


def kernel(
    z, tok_ref, cot_ref, routes_ref, rc_ref, gate_ref, up_ref, down_ref,
    tg_out, gate_out, up_out, down_out, gsq_out, usq_out, dsq_out, rout_out,
    s_mat, t_mat, s1m, r1m, s1, r1, s2m, x2m, s2, x2, y2m, y2,
    gacc, uacc, pacc, dcat, hid, wcol, wp, wpr, pts, ptr, pto,
    s3m, r3m, s3, r3, s4m, r4m, s4, r4, sq, sqr, term, trec, tsum, tsumr,
    z1s, z1r, p2s, p2r, fs, fr, ptsm, ptrm, r3s, r3r, r4s, r4r, ms, mr, ts, tr,
):
    e, t = lax.axis_index("ep"), lax.axis_index("tp")
    g, p = e // z.gs, e % z.gs
    other = 1 - t

    def rcopy(src, dst, ss, rs, ep, tp):
        return pltpu.make_async_remote_copy(
            src_ref=src, dst_ref=dst, send_sem=ss, recv_sem=rs,
            device_id=(ep, tp), device_id_type=MESH,
        )

    barrier = pltpu.get_barrier_semaphore()
    for d in range(1, z.n_ep):
        pl.semaphore_signal(
            barrier, inc=1, device_id=((e + d) % z.n_ep, t), device_id_type=MESH
        )
    pl.semaphore_signal(barrier, inc=1, device_id=(e, other), device_id_type=MESH)

    sends = []

    def grows(h):
        return pl.ds(pl.multiple_of(h * z.gr, z.gr), z.gr)

    def prows(q):
        return pl.ds(pl.multiple_of(q * z.sl, z.sl), z.sl)

    def group_send(src, dst, ss, rs, c):
        for d in range(1, z.groups):
            h = (g + d) % z.groups
            cp = rcopy(src.at[grows(h)], dst.at[grows(g)], ss.at[c, d], rs.at[c, d], h * z.gs + p, t)
            cp.start()
            sends.append(cp)
        dst[grows(g), :] = src[grows(g), :]

    def group_wait(src, dst, ss, rs, c):
        for d in range(1, z.groups):
            h = (g + z.groups - d) % z.groups
            rcopy(src.at[grows(h)], dst.at[grows(h)], ss.at[c, d], rs.at[c, d], h * z.gs + p, t).wait_recv()

    def plane_send(src, dst, ss, rs, c):
        for d in range(1, z.gs):
            q = (p + d) % z.gs
            cp = rcopy(src.at[prows(q)], dst.at[prows(p)], ss.at[c, d], rs.at[c, d], g * z.gs + q, t)
            cp.start()
            sends.append(cp)
        dst[prows(p), :] = src[prows(p), :]

    def plane_wait_one(src, dst, ss, rs, c, d):
        q = (p + z.gs - d) % z.gs
        rcopy(src.at[prows(q)], dst.at[prows(q)], ss.at[c, d], rs.at[c, d], g * z.gs + q, t).wait_recv()

    def plane_wait(src, dst, ss, rs, c):
        for d in range(1, z.gs):
            plane_wait_one(src, dst, ss, rs, c, d)

    def pair_send(src, dst, ss, rs):
        cp = rcopy(src, dst, ss, rs, e, other)
        cp.start()
        sends.append(cp)
        return cp

    tok = tok_ref[...]
    logits = mm(tok, rc_ref[...], 1, 1)
    lane = lanes_of((z.rows, z.rl))
    r0, r1_ = routes_ref[:, 0:1], routes_ref[:, 1:2]
    chosen = (lane == r0) | (lane == r1_)
    low = (lane - z.experts) * z.gs
    is_group = (lane >= z.experts) & (lane < z.experts + z.groups)
    in_group = is_group & (r0 >= low) & (r0 < low + z.gs)
    expd = jnp.exp(logits)
    gexp = jnp.where(is_group, expd, 0.0)
    gprob = gexp / jnp.sum(gexp, axis=1, keepdims=True)
    picked = jnp.sum(jnp.where(in_group, gprob, 0.0), axis=1, keepdims=True)
    pexp = jnp.where(chosen, expd, 0.0)
    paired = pexp / jnp.sum(pexp, axis=1, keepdims=True)
    meta = jnp.where(chosen, jnp.maximum(picked * paired, TINY), 0.0).astype(BF)

    def before(n):
        return (lanes_of((n, n), 1) < lanes_of((n, n), 0)).astype(F32).astype(BF)

    ghot = in_group.astype(F32)
    grank = mm(before(z.rows), ghot.astype(BF))
    grank = jnp.where(in_group, grank, -1.0).astype(BF)
    er, el = lanes_of((z.rl, z.r1), 0) - z.experts, lanes_of((z.rl, z.r1), 1)
    expand = ((el >= er * z.gr) & (el < (er + 1) * z.gr)).astype(F32).astype(BF)
    place = (lanes_of((z.rows, z.r1)) & (z.gr - 1)).astype(F32)
    s_mat[...] = (mm(grank, expand) == place).astype(F32).astype(BF)

    s1m[...] = mm(s_mat[...], meta, 0, 0).astype(BF)
    pl.semaphore_wait(barrier, z.n_ep)
    group_send(s1m, r1m, z1s, z1r, z.nc)

    def cols_at(half, k):
        return pl.ds(pl.multiple_of(half * z.cw + k * z.cc, z.cc), z.cc)

    for c in range(z.nc):
        src = tok_ref if c < z.half_chunks else cot_ref
        s1[c] = mm(s_mat[...], src[:, cols_at(t, c % z.half_chunks)], 0, 0).astype(BF)
        group_send(s1.at[c], r1.at[c], z1s, z1r, c)

    group_wait(s1m, r1m, z1s, z1r, z.nc)
    vals = r1m[...]
    lane1 = lanes_of((z.r1, z.rl))
    member = (vals.astype(F32) > 0.0) & (lane1 < z.experts)
    rank = mm(before(z.r1), member.astype(F32).astype(BF))
    rank = jnp.where(member, rank, -1.0).astype(BF)
    er, el = lanes_of((z.rl, z.pairs), 0) - g * z.gs, lanes_of((z.rl, z.pairs), 1)
    expand = ((el >= er * z.sl) & (el < (er + 1) * z.sl)).astype(F32).astype(BF)
    place = (lanes_of((z.r1, z.pairs)) & (z.sl - 1)).astype(F32)
    t_mat[...] = (mm(rank, expand) == place).astype(F32).astype(BF)
    s2m[...] = mm(t_mat[...], vals, 0, 0).astype(BF)
    plane_send(s2m, x2m, p2s, p2r, z.nc)

    def pack_two(c):
        group_wait(s1.at[c], r1.at[c], z1s, z1r, c)
        s2[c] = mm(t_mat[...], r1[c], 0, 0).astype(BF)
        plane_send(s2.at[c], x2.at[c], p2s, p2r, c)
        pair_send(x2.at[c, prows(p)], y2.at[c, prows(p)], fs.at[c, 0], fr.at[c, 0])

    def accumulate(x, half, c):
        if c < z.half_chunks:
            at = cols_at(half, c)
            gate_add, up_add = mm(x, gate_ref[at, :]), mm(x, up_ref[at, :])
            gacc[...] += gate_add
            uacc[...] += up_add
        else:
            pacc[...] += mm(x, down_ref[:, cols_at(half, c - z.half_chunks)], 1, 1)

    def land(c):
        for d in range(1, z.gs):
            plane_wait_one(s2.at[c], x2.at[c], p2s, p2r, c, d)
            q = (p + z.gs - d) % z.gs
            pair_send(x2.at[c, prows(q)], y2.at[c, prows(q)], fs.at[c, d], fr.at[c, d])
        accumulate(x2[c], t, c)

    def land_other(c):
        for d in range(z.gs):
            q = (p + z.gs - d) % z.gs
            rcopy(x2.at[c, prows(q)], y2.at[c, prows(q)], fs.at[c, d], fr.at[c, d], e, other).wait_recv()
        accumulate(y2[c], other, c)

    gacc[...] = jnp.zeros_like(gacc)
    uacc[...] = jnp.zeros_like(uacc)
    pacc[...] = jnp.zeros_like(pacc)
    for c in range(z.nc + 2):
        if c < z.nc:
            pack_two(c)
        if 1 <= c <= z.nc:
            land(c - 1)
        if c >= 2:
            land_other(c - 2)
    plane_wait(s2m, x2m, p2s, p2r, z.nc)

    lane2 = lanes_of((z.pairs, z.rl))
    val = jnp.sum(jnp.where(lane2 == e, x2m[...].astype(F32), 0.0), axis=1, keepdims=True)
    scale = jnp.where(val > TINY, val, 0.0)
    wcol[...] = jnp.broadcast_to(scale, wcol.shape)
    gate_pre, up_pre, pulled = gacc[...], uacc[...], pacc[...]
    sig = 1.0 / (1.0 + jnp.exp(-gate_pre))
    silu = gate_pre * sig
    hidden = (silu * up_pre).astype(BF)
    hid[...] = hidden
    wp[...] = jnp.broadcast_to(
        jnp.sum(pulled * hidden.astype(F32), axis=1, keepdims=True), wp.shape
    )
    w_copy = pair_send(wp, wpr, ms.at[0], mr.at[0])
    dh = scale * pulled
    dcat[:, : z.ff] = (dh * up_pre * sig * (1.0 + gate_pre * (1.0 - sig))).astype(BF)
    dcat[:, z.ff :] = (dh * silu).astype(BF)

    def token_term(half, k):
        at = cols_at(half, k)
        return (
            mm(dcat[:, : z.ff], gate_ref[at, :], 1, 1) + mm(dcat[:, z.ff :], up_ref[at, :], 1, 1)
        ).astype(BF)

    pt = []
    for k in range(z.half_chunks):
        pts[k] = token_term(other, k)
        pt.append(pair_send(pts.at[k], ptr.at[k], ptsm.at[k], ptrm.at[k]))
    w_copy.wait_recv()
    wsum = wp[:, 0:1] + wpr[:, 0:1]
    s3m[...] = jnp.where(lane2 == e, wsum, 0.0).astype(BF)
    plane_send(s3m, r3m, r3s, r3r, z.half_chunks)
    for k in range(z.half_chunks):
        pto[k] = token_term(t, k)
        pt[k].wait_recv()
        s3[k] = (pto[k].astype(F32) + ptr[k].astype(F32)).astype(BF)
        plane_send(s3.at[k], r3.at[k], r3s, r3r, k)

    ones_ff = jnp.ones((16, z.ff), BF)

    def gate_up_grads(xs, half, k):
        at = cols_at(half, k)
        total = mm(xs[k], dcat[...], 0, 0)
        gate_out[at, :] = total[:, : z.ff].astype(BF)
        up_out[at, :] = total[:, z.ff :].astype(BF)
        square = (total * total).astype(BF)
        sq[0:1, at] = mm(ones_ff, square[:, : z.ff], 1, 1)[0:1]
        sq[1:2, at] = mm(ones_ff, square[:, z.ff :], 1, 1)[0:1]

    def down_grads(xs, half, k):
        scaled = (wcol[:, 0:1] * xs[z.half_chunks + k].astype(F32)).astype(BF)
        total = mm(hid[...], scaled, 0, 0)
        down_out[:, cols_at(half, k)] = total.astype(BF)
        return mm(jnp.ones((16, z.cc), BF), (total * total).astype(BF), 1, 1)[0:1]

    def back_two(k):
        plane_wait(s3.at[k], r3.at[k], r3s, r3r, k)
        s4[k] = mm(t_mat[...], r3[k]).astype(BF)
        group_send(s4.at[k], r4.at[k], r4s, r4r, k)

    gate_up_grads(x2, t, 0)
    plane_wait(s3m, r3m, r3s, r3r, z.half_chunks)
    s4m[...] = mm(t_mat[...], r3m[...]).astype(BF)
    group_send(s4m, r4m, r4s, r4r, z.half_chunks)
    gate_up_grads(x2, t, 1)
    gate_up_grads(y2, other, 0)
    back_two(0)
    gate_up_grads(y2, other, 1)
    sq_copy = pair_send(sq, sqr, ms.at[1], mr.at[1])

    group_wait(s4m, r4m, r4s, r4r, z.half_chunks)
    dw = mm(s_mat[...], r4m[...])
    dpicked = jnp.sum(dw * paired, axis=1, keepdims=True)
    q = picked * dw
    dchosen = paired * (q - jnp.sum(paired * q, axis=1, keepdims=True))
    dgroup = jnp.where(is_group, (dpicked * picked) * (ghot - gprob), 0.0)
    dall = (dchosen + dgroup).astype(BF)
    dterm = dall[:, : z.rw] if z.rw < z.rl else dall
    tcopies = []
    if z.reduce_here:
        full = mm(dterm, tok_ref[...], 0, 0)
        for i in range(z.n_ep):
            term[i] = full[:, i * z.ch : (i + 1) * z.ch]

        def term_copy(m):
            to = (e + 2 * m + t) % z.n_ep
            return rcopy(term.at[to], trec.at[m], ts.at[m], tr.at[m], to, t)

        @pl.when(t == 0)
        def _():
            trec[0] = term[e]

        @pl.when(t == 1)
        def _():
            term_copy(0).start()

        for m in range(1, z.n_ep // 2):
            term_copy(m).start()
    else:
        row = lanes_of((z.rows, z.rl), 0)[:, : dterm.shape[1]]
        mine = (row >= t * (z.rows // 2)) & (row < (t + 1) * (z.rows // 2))
        dterm = jnp.where(mine, dterm.astype(F32), 0.0).astype(BF)
        rout_out[...] = mm(dterm, tok_ref[...], 0, 0)

    back_two(1)
    dsq = down_grads(x2, t, 0)
    dsq += down_grads(x2, t, 1)
    dsq += down_grads(y2, other, 0)

    if z.reduce_here:

        @pl.when(t == 1)
        def _():
            term_copy(0).wait_recv()

        for m in range(1, z.n_ep // 2):
            term_copy(m).wait_recv()
        acc = trec[0]
        for m in range(1, z.n_ep // 2):
            acc = acc + trec[m]
        tsum[...] = acc
        t_pair = pair_send(tsum, tsumr, ms.at[2], mr.at[2])
    dsq += down_grads(y2, other, 1)
    dsq_out[...] = dsq

    for k in range(z.half_chunks):
        group_wait(s4.at[k], r4.at[k], r4s, r4r, k)
        tg_out[:, k * z.cc : (k + 1) * z.cc] = (
            mm(s_mat[...], r4[k]) + mm(dall, rc_ref[:, cols_at(t, k)])
        ).astype(BF)
    sq_copy.wait_recv()
    gsq_out[...] = sq[0:1, :] + sqr[0:1, :]
    usq_out[...] = sq[1:2, :] + sqr[1:2, :]
    if z.reduce_here:
        t_pair.wait_recv()
        rout_out[...] = tsum[...] + tsumr[...]

        @pl.when(t == 1)
        def _():
            term_copy(0).wait_send()

        for m in range(1, z.n_ep // 2):
            term_copy(m).wait_send()
    for cp in sends:
        cp.wait_send()


def body(axes, tokens, cotangent, routes, router_group, router_expert, gate_proj, up_proj, down_proj):
    z = sizes_of(axes, tokens, routes, router_group, router_expert, gate_proj)
    rc = jnp.concatenate([router_expert.T, router_group.T], axis=0)
    rc = jnp.pad(rc, ((0, z.rl - rc.shape[0]), (0, 0)))
    h, nc, cc = z.half_chunks, z.nc, z.cc
    rout_shape = (z.rw, z.ch) if z.reduce_here else (min(z.rw, z.rl), z.width)
    outs = [
        ((z.rows, z.cw), BF), ((z.width, z.ff), BF), ((z.width, z.ff), BF), ((z.ff, z.width), BF),
        ((1, z.width), F32), ((1, z.width), F32), ((1, z.ff), F32), (rout_shape, F32),
    ]
    V = pltpu.VMEM
    chd = z.ch if z.reduce_here else 128
    scratch = [
        V((z.rows, z.r1), BF), V((z.r1, z.pairs), BF),
        V((z.r1, z.rl), BF), V((z.r1, z.rl), BF),
        V((nc, z.r1, cc), BF), V((nc, z.r1, cc), BF),
        V((z.pairs, z.rl), BF), V((z.pairs, z.rl), BF),
        V((nc, z.pairs, cc), BF), V((nc, z.pairs, cc), BF),
        V((8, 128), BF), V((nc, z.pairs, cc), BF),
        V((z.pairs, z.ff), F32), V((z.pairs, z.ff), F32), V((z.pairs, z.ff), F32),
        V((z.pairs, 2 * z.ff), BF), V((z.pairs, z.ff), BF), V((z.pairs, 128), F32),
        V((z.pairs, 128), F32), V((z.pairs, 128), F32),
        V((h, z.pairs, cc), BF), V((h, z.pairs, cc), BF), V((h, z.pairs, cc), BF),
        V((z.pairs, z.rl), BF), V((z.pairs, z.rl), BF),
        V((h, z.pairs, cc), BF), V((h, z.pairs, cc), BF),
        V((z.r1, z.rl), BF), V((z.r1, z.rl), BF),
        V((h, z.r1, cc), BF), V((h, z.r1, cc), BF),
        V((2, z.width), F32), V((2, z.width), F32),
        V((z.n_ep, z.rw, chd), F32), V((z.n_ep // 2, z.rw, chd), F32),
        V((z.rw, chd), F32), V((z.rw, chd), F32),
    ]
    D = pltpu.SemaphoreType.DMA
    sems = [
        D((nc + 1, z.groups)), D((nc + 1, z.groups)), D((nc + 1, z.gs)), D((nc + 1, z.gs)),
        D((nc, z.gs)), D((nc, z.gs)), D((h,)), D((h,)),
        D((h + 1, z.gs)), D((h + 1, z.gs)), D((h + 1, z.groups)), D((h + 1, z.groups)),
        D((3,)), D((3,)), D((z.n_ep // 2,)), D((z.n_ep // 2,)),
    ]
    spec = pl.BlockSpec(memory_space=pltpu.VMEM)
    tg, gate, up, down, gsq, usq, dsq, rout = pl.pallas_call(
        functools.partial(kernel, z),
        out_shape=[jax.ShapeDtypeStruct(s, d) for s, d in outs],
        in_specs=[spec] * 7,
        out_specs=[spec] * len(outs),
        scratch_shapes=scratch + sems,
        compiler_params=pltpu.CompilerParams(
            collective_id=0, has_side_effects=True, vmem_limit_bytes=60 * 2**20
        ),
    )(tokens, cotangent, routes, rc, gate_proj[0], up_proj[0], down_proj[0])
    own = z.width // (z.n_ep * z.n_tp)
    if z.reduce_here:
        mine = lax.dynamic_slice_in_dim(rout, lax.axis_index("tp") * own, own, 1).T
    else:
        mine = lax.psum_scatter(rout.T, ("ep", "tp"), scatter_dimension=0, tiled=True)
    reg = mine[:, : z.experts]
    rgg = mine[:, z.experts : z.experts + z.groups]
    rrows = jnp.sum(reg * reg, axis=1) + jnp.sum(rgg * rgg, axis=1)
    return (tg, gate[None], up[None], down[None], gsq, usq, dsq, reg, rgg, rrows)


def solution(mesh):
    return jax.shard_map(
        functools.partial(body, dict(mesh.shape)),
        mesh=mesh,
        in_specs=(
            P("ep", None), P("ep", None), P("ep", None), P(), P(),
            P("ep", None, "tp"), P("ep", None, "tp"), P("ep", "tp", None),
        ),
        out_specs=(
            P("ep", "tp"), P("ep", None, "tp"), P("ep", None, "tp"), P("ep", "tp", None),
            P("ep", None), P("ep", None), P("ep", "tp"),
            P(("ep", "tp"), None), P(("ep", "tp"), None), P(("ep", "tp")),
        ),
        check_vma=False,
    )
```

```python
import functools

import jax
import jax.numpy as jnp
from jax import lax
from jax.experimental import pallas as pl
from jax.experimental.pallas import tpu as pltpu
from jax.sharding import PartitionSpec as P

MESH = pl.DeviceIdType.MESH
BF = jnp.bfloat16
F32 = jnp.float32


def mm(a, b, da=1, db=0):
    return lax.dot_general(a, b, (((da,), (db,)), ((), ())), preferred_element_type=F32)


def lanes_of(shape, dim=1):
    return lax.broadcasted_iota(jnp.int32, shape, dim)


class Sizes:
    pass


def sizes_of(mesh, tokens, routes, router_group, router_expert, gate_proj):
    z = Sizes()
    z.n_ep, z.n_tp = mesh["ep"], mesh["tp"]
    z.rows, z.width = tokens.shape
    z.top = routes.shape[1]
    z.groups, z.experts = router_group.shape[1], router_expert.shape[1]
    z.gs = z.experts // z.groups
    z.cap = z.rows // z.gs
    z.gr = z.gs * z.cap // z.top
    z.r1 = z.groups * z.gr
    z.sl = z.groups * z.cap
    z.pairs = z.gs * z.sl
    z.ff = gate_proj.shape[2]
    z.cw = z.width // z.n_tp
    z.half_chunks = 4
    z.nc = 2 * z.half_chunks
    z.cc = z.cw // z.half_chunks
    z.rl = -(-(z.experts + z.groups) // 128) * 128
    z.rw = -(-(z.experts + z.groups) // 8) * 8
    z.ch = z.width // z.n_ep
    z.reduce_here = z.ch % 128 == 0 and z.n_ep % 2 == 0
    assert z.experts == z.n_ep and z.n_tp == 2 and z.top == 2
    assert z.sl & (z.sl - 1) == 0 and z.gr & (z.gr - 1) == 0
    return z


def kernel(
    z, tok_ref, cot_ref, routes_ref, rexp_ref, rgrp_ref, gate_ref, up_ref, down_ref,
    tg_out, gate_out, up_out, down_out, gsq_out, usq_out, dsq_out, rout_out,
    rc_ref, s1w, r1w,
    s_mat, t_mat, s1m, r1m, s1, r1, s2m, x2m, s2, x2, y2m, y2,
    gacc, uacc, pacc, dcat, hid, wcol, wp, wpr, pts, ptr, pto,
    s3m, r3m, s3, r3, s4m, r4m, s4, r4, sq, sqr, term, trec, tsum, tsumr,
    z1s, z1r, p2s, p2r, fs, fr, ptsm, ptrm, r3s, r3r, r4s, r4r, ms, mr, ts, tr,
):
    e, t = lax.axis_index("ep"), lax.axis_index("tp")
    g, p = e // z.gs, e % z.gs
    other = 1 - t

    def rcopy(src, dst, ss, rs, ep, tp):
        return pltpu.make_async_remote_copy(
            src_ref=src, dst_ref=dst, send_sem=ss, recv_sem=rs,
            device_id=(ep, tp), device_id_type=MESH,
        )

    barrier = pltpu.get_barrier_semaphore()
    for d in range(1, z.n_ep):
        pl.semaphore_signal(
            barrier, inc=1, device_id=((e + d) % z.n_ep, t), device_id_type=MESH
        )
    pl.semaphore_signal(barrier, inc=1, device_id=(e, other), device_id_type=MESH)

    sends = []

    def grows(h):
        return pl.ds(pl.multiple_of(h * z.gr, z.gr), z.gr)

    def prows(q):
        return pl.ds(pl.multiple_of(q * z.sl, z.sl), z.sl)

    def group_send(src, dst, ss, rs, c):
        for d in range(1, z.groups):
            h = (g + d) % z.groups
            cp = rcopy(src.at[grows(h)], dst.at[grows(g)], ss.at[c, d], rs.at[c, d], h * z.gs + p, t)
            cp.start()
            sends.append(cp)
        dst[grows(g), :] = src[grows(g), :]

    def group_wait(src, dst, ss, rs, c):
        for d in range(1, z.groups):
            h = (g + z.groups - d) % z.groups
            rcopy(src.at[grows(h)], dst.at[grows(h)], ss.at[c, d], rs.at[c, d], h * z.gs + p, t).wait_recv()

    def plane_send(src, dst, ss, rs, c):
        for d in range(1, z.gs):
            q = (p + d) % z.gs
            cp = rcopy(src.at[prows(q)], dst.at[prows(p)], ss.at[c, d], rs.at[c, d], g * z.gs + q, t)
            cp.start()
            sends.append(cp)
        dst[prows(p), :] = src[prows(p), :]

    def plane_wait_one(src, dst, ss, rs, c, d):
        q = (p + z.gs - d) % z.gs
        rcopy(src.at[prows(q)], dst.at[prows(q)], ss.at[c, d], rs.at[c, d], g * z.gs + q, t).wait_recv()

    def plane_wait(src, dst, ss, rs, c):
        for d in range(1, z.gs):
            plane_wait_one(src, dst, ss, rs, c, d)

    def pair_send(src, dst, ss, rs):
        cp = rcopy(src, dst, ss, rs, e, other)
        cp.start()
        sends.append(cp)
        return cp

    lane = lanes_of((z.rows, z.rl))
    eye = lanes_of((z.rows, z.rows), 0) == lanes_of((z.rows, z.rows), 1)

    def column(row):
        return jnp.sum(jnp.where(eye, row.astype(F32), 0.0), axis=1, keepdims=True).astype(jnp.int32)

    r0, r1_ = column(routes_ref[0:1, :]), column(routes_ref[1:2, :])
    chosen = (lane == r0) | (lane == r1_)
    low = (lane - z.experts) * z.gs
    is_group = (lane >= z.experts) & (lane < z.experts + z.groups)
    in_group = is_group & (r0 >= low) & (r0 < low + z.gs)

    def before(n):
        return (lanes_of((n, n), 1) < lanes_of((n, n), 0)).astype(F32).astype(BF)

    ghot = in_group.astype(F32)
    grank = mm(before(z.rows), ghot.astype(BF))
    grank = jnp.where(in_group, grank, -1.0).astype(BF)
    er, el = lanes_of((z.rl, z.r1), 0) - z.experts, lanes_of((z.rl, z.r1), 1)
    expand = ((el >= er * z.gr) & (el < (er + 1) * z.gr)).astype(F32).astype(BF)
    place = (lanes_of((z.rows, z.r1)) & (z.gr - 1)).astype(F32)
    s_mat[...] = (mm(grank, expand) == place).astype(F32).astype(BF)

    s1m[...] = mm(s_mat[...], chosen.astype(F32).astype(BF), 0, 0).astype(BF)
    pl.semaphore_wait(barrier, z.n_ep)
    group_send(s1m, r1m, z1s, z1r, z.nc)

    def cols_at(half, k):
        return pl.ds(pl.multiple_of(half * z.cw + k * z.cc, z.cc), z.cc)

    for c in range(z.nc):
        src = tok_ref if c < z.half_chunks else cot_ref
        s1[c] = mm(s_mat[...], src[:, cols_at(t, c % z.half_chunks)], 0, 0).astype(BF)
        group_send(s1.at[c], r1.at[c], z1s, z1r, c)

    rc_ref[...] = jnp.zeros_like(rc_ref)
    rc_ref[0 : z.experts, :] = rexp_ref[...]
    rc_ref[z.experts : z.experts + z.groups, :] = rgrp_ref[...]
    expd = jnp.exp(mm(tok_ref[...], rc_ref[...], 1, 1))
    gexp = jnp.where(is_group, expd, 0.0)
    gprob = gexp / jnp.sum(gexp, axis=1, keepdims=True)
    picked = jnp.sum(jnp.where(in_group, gprob, 0.0), axis=1, keepdims=True)
    pexp = jnp.where(chosen, expd, 0.0)
    paired = pexp / jnp.sum(pexp, axis=1, keepdims=True)
    s1w[...] = mm(s_mat[...], (picked * paired).astype(BF), 0, 0).astype(BF)
    group_send(s1w, r1w, z1s, z1r, z.nc + 1)

    group_wait(s1m, r1m, z1s, z1r, z.nc)
    vals = r1m[...]
    lane1 = lanes_of((z.r1, z.rl))
    member = (vals.astype(F32) > 0.0) & (lane1 < z.experts)
    rank = mm(before(z.r1), member.astype(F32).astype(BF))
    rank = jnp.where(member, rank, -1.0).astype(BF)
    er, el = lanes_of((z.rl, z.pairs), 0) - g * z.gs, lanes_of((z.rl, z.pairs), 1)
    expand = ((el >= er * z.sl) & (el < (er + 1) * z.sl)).astype(F32).astype(BF)
    place = (lanes_of((z.r1, z.pairs)) & (z.sl - 1)).astype(F32)
    t_mat[...] = (mm(rank, expand) == place).astype(F32).astype(BF)

    def pack_two(c):
        group_wait(s1.at[c], r1.at[c], z1s, z1r, c)
        s2[c] = mm(t_mat[...], r1[c], 0, 0).astype(BF)
        plane_send(s2.at[c], x2.at[c], p2s, p2r, c)
        pair_send(x2.at[c, prows(p)], y2.at[c, prows(p)], fs.at[c, 0], fr.at[c, 0])

    def accumulate(x, half, c):
        if c < z.half_chunks:
            at = cols_at(half, c)
            gate_add, up_add = mm(x, gate_ref[at, :]), mm(x, up_ref[at, :])
            gacc[...] += gate_add
            uacc[...] += up_add
        else:
            pacc[...] += mm(x, down_ref[:, cols_at(half, c - z.half_chunks)], 1, 1)

    def land(c):
        for d in range(1, z.gs):
            plane_wait_one(s2.at[c], x2.at[c], p2s, p2r, c, d)
            q = (p + z.gs - d) % z.gs
            pair_send(x2.at[c, prows(q)], y2.at[c, prows(q)], fs.at[c, d], fr.at[c, d])
        accumulate(x2[c], t, c)

    def land_other(c):
        for d in range(z.gs):
            q = (p + z.gs - d) % z.gs
            rcopy(x2.at[c, prows(q)], y2.at[c, prows(q)], fs.at[c, d], fr.at[c, d], e, other).wait_recv()
        accumulate(y2[c], other, c)

    gacc[...] = jnp.zeros_like(gacc)
    uacc[...] = jnp.zeros_like(uacc)
    pacc[...] = jnp.zeros_like(pacc)
    for c in range(z.nc + 3):
        if c < z.nc:
            pack_two(c)
        if c == z.nc - 1:
            group_wait(s1w, r1w, z1s, z1r, z.nc + 1)
            s2m[...] = mm(t_mat[...], r1w[...], 0, 0).astype(BF)
            plane_send(s2m, x2m, p2s, p2r, z.nc)
        if 2 <= c < z.nc + 2:
            land(c - 2)
        if c >= 3:
            land_other(c - 3)
    plane_wait(s2m, x2m, p2s, p2r, z.nc)

    lane2 = lanes_of((z.pairs, z.rl))
    scale = jnp.sum(jnp.where(lane2 == e, x2m[...].astype(F32), 0.0), axis=1, keepdims=True)
    wcol[...] = jnp.broadcast_to(scale, wcol.shape)
    gate_pre, up_pre, pulled = gacc[...], uacc[...], pacc[...]
    sig = 1.0 / (1.0 + jnp.exp(-gate_pre))
    silu = gate_pre * sig
    hidden = (silu * up_pre).astype(BF)
    hid[...] = hidden
    wp[...] = jnp.broadcast_to(
        jnp.sum(pulled * hidden.astype(F32), axis=1, keepdims=True), wp.shape
    )
    w_copy = pair_send(wp, wpr, ms.at[0], mr.at[0])
    dh = scale * pulled
    dcat[:, : z.ff] = (dh * up_pre * sig * (1.0 + gate_pre * (1.0 - sig))).astype(BF)
    dcat[:, z.ff :] = (dh * silu).astype(BF)

    def token_term(half, k):
        at = cols_at(half, k)
        return (
            mm(dcat[:, : z.ff], gate_ref[at, :], 1, 1) + mm(dcat[:, z.ff :], up_ref[at, :], 1, 1)
        ).astype(BF)

    pt = []
    for k in range(z.half_chunks):
        pts[k] = token_term(other, k)
        pt.append(pair_send(pts.at[k], ptr.at[k], ptsm.at[k], ptrm.at[k]))
    w_copy.wait_recv()
    wsum = wp[:, 0:1] + wpr[:, 0:1]
    s3m[...] = jnp.where(lane2 == e, wsum, 0.0).astype(BF)
    plane_send(s3m, r3m, r3s, r3r, z.half_chunks)
    for k in range(z.half_chunks):
        pto[k] = token_term(t, k)
        pt[k].wait_recv()
        s3[k] = (pto[k].astype(F32) + ptr[k].astype(F32)).astype(BF)
        plane_send(s3.at[k], r3.at[k], r3s, r3r, k)

    ones_ff = jnp.ones((16, z.ff), BF)

    def gate_up_grads(xs, half, k):
        at = cols_at(half, k)
        total = mm(xs[k], dcat[...], 0, 0)
        gate_out[at, :] = total[:, : z.ff].astype(BF)
        up_out[at, :] = total[:, z.ff :].astype(BF)
        square = (total * total).astype(BF)
        sq[0:1, at] = mm(ones_ff, square[:, : z.ff], 1, 1)[0:1]
        sq[1:2, at] = mm(ones_ff, square[:, z.ff :], 1, 1)[0:1]

    def down_grads(xs, half, k):
        scaled = (wcol[:, 0:1] * xs[z.half_chunks + k].astype(F32)).astype(BF)
        total = mm(hid[...], scaled, 0, 0)
        down_out[:, cols_at(half, k)] = total.astype(BF)
        return mm(jnp.ones((16, z.cc), BF), (total * total).astype(BF), 1, 1)[0:1]

    def back_two(k):
        plane_wait(s3.at[k], r3.at[k], r3s, r3r, k)
        s4[k] = mm(t_mat[...], r3[k]).astype(BF)
        group_send(s4.at[k], r4.at[k], r4s, r4r, k)

    gate_up_grads(x2, t, 0)
    plane_wait(s3m, r3m, r3s, r3r, z.half_chunks)
    s4m[...] = mm(t_mat[...], r3m[...]).astype(BF)
    group_send(s4m, r4m, r4s, r4r, z.half_chunks)
    gate_up_grads(x2, t, 1)
    for k in range(z.half_chunks - 1):
        back_two(k)
        if k + 2 < z.half_chunks:
            gate_up_grads(x2, t, k + 2)
        else:
            gate_up_grads(y2, other, 0)

    group_wait(s4m, r4m, r4s, r4r, z.half_chunks)
    dw = mm(s_mat[...], r4m[...])
    dpicked = jnp.sum(dw * paired, axis=1, keepdims=True)
    q = picked * dw
    dchosen = paired * (q - jnp.sum(paired * q, axis=1, keepdims=True))
    dgroup = jnp.where(is_group, (dpicked * picked) * (ghot - gprob), 0.0)
    dall = (dchosen + dgroup).astype(BF)
    dterm = dall[:, : z.rw] if z.rw < z.rl else dall
    tcopies = []
    if z.reduce_here:
        full = mm(dterm, tok_ref[...], 0, 0)
        for i in range(z.n_ep):
            term[i] = full[:, i * z.ch : (i + 1) * z.ch]

        def term_copy(m):
            to = (e + 2 * m + t) % z.n_ep
            return rcopy(term.at[to], trec.at[m], ts.at[m], tr.at[m], to, t)

        @pl.when(t == 0)
        def _():
            trec[0] = term[e]

        @pl.when(t == 1)
        def _():
            term_copy(0).start()

        for m in range(1, z.n_ep // 2):
            term_copy(m).start()
    else:
        row = lanes_of((z.rows, z.rl), 0)[:, : dterm.shape[1]]
        mine = (row >= t * (z.rows // 2)) & (row < (t + 1) * (z.rows // 2))
        dterm = jnp.where(mine, dterm.astype(F32), 0.0).astype(BF)
        rout_out[...] = mm(dterm, tok_ref[...], 0, 0)

    back_two(z.half_chunks - 1)
    for k in range(1, z.half_chunks):
        gate_up_grads(y2, other, k)
    sq_copy = pair_send(sq, sqr, ms.at[1], mr.at[1])
    dsq = jnp.zeros((1, z.ff), F32)
    for k in range(z.half_chunks):
        dsq += down_grads(x2, t, k)

    if z.reduce_here:

        @pl.when(t == 1)
        def _():
            term_copy(0).wait_recv()

        for m in range(1, z.n_ep // 2):
            term_copy(m).wait_recv()
        acc = trec[0]
        for m in range(1, z.n_ep // 2):
            acc = acc + trec[m]
        tsum[...] = acc
        t_pair = pair_send(tsum, tsumr, ms.at[2], mr.at[2])
    for k in range(z.half_chunks):
        dsq += down_grads(y2, other, k)
    dsq_out[...] = dsq

    for k in range(z.half_chunks):
        group_wait(s4.at[k], r4.at[k], r4s, r4r, k)
        tg_out[:, k * z.cc : (k + 1) * z.cc] = (
            mm(s_mat[...], r4[k]) + mm(dall, rc_ref[:, cols_at(t, k)])
        ).astype(BF)
    sq_copy.wait_recv()
    gsq_out[...] = sq[0:1, :] + sqr[0:1, :]
    usq_out[...] = sq[1:2, :] + sqr[1:2, :]
    if z.reduce_here:
        t_pair.wait_recv()
        rout_out[...] = tsum[...] + tsumr[...]

        @pl.when(t == 1)
        def _():
            term_copy(0).wait_send()

        for m in range(1, z.n_ep // 2):
            term_copy(m).wait_send()
    for cp in sends:
        cp.wait_send()


def finish(
    z, gate_in, up_in, down_in, tg_in, gsq_in, usq_in, dsq_in, rout_in,
    gate_out, up_out, down_out, tg_out, gsq_out, usq_out, dsq_out, reg_out, rgg_out, rows_out, sem,
):
    copies = []
    pairs = (
        (gate_in, gate_out), (up_in, up_out), (down_in, down_out), (tg_in, tg_out),
        (gsq_in, gsq_out), (usq_in, usq_out), (dsq_in, dsq_out),
    )
    for i, (src, dst) in enumerate(pairs):
        cp = pltpu.make_async_copy(src, dst, sem.at[i])
        cp.start()
        copies.append(cp)
    half = z.ch // 2
    both = rout_in[...]
    mine = jnp.where(lax.axis_index("tp") == 0, both[:, :half], both[:, half:])
    reg = mine[: z.experts]
    rgg = mine[z.experts : z.experts + z.groups]
    reg_out[...] = reg
    rgg_out[...] = rgg
    rows_out[...] = jnp.sum(reg * reg, axis=0, keepdims=True) + jnp.sum(rgg * rgg, axis=0, keepdims=True)
    for cp in copies:
        cp.wait()


def body(axes, tokens, cotangent, routes, router_group, router_expert, gate_proj, up_proj, down_proj):
    z = sizes_of(axes, tokens, routes, router_group, router_expert, gate_proj)
    h, nc, cc = z.half_chunks, z.nc, z.cc
    rout_shape = (z.rw, z.ch) if z.reduce_here else (min(z.rw, z.rl), z.width)
    outs = [
        ((z.rows, z.cw), BF), ((z.width, z.ff), BF), ((z.width, z.ff), BF), ((z.ff, z.width), BF),
        ((1, z.width), F32), ((1, z.width), F32), ((1, z.ff), F32), (rout_shape, F32),
    ]
    V = pltpu.VMEM
    chd = z.ch if z.reduce_here else 128
    scratch = [
        V((z.rl, z.width), BF), V((z.r1, z.rl), BF), V((z.r1, z.rl), BF),
        V((z.rows, z.r1), BF), V((z.r1, z.pairs), BF),
        V((z.r1, z.rl), BF), V((z.r1, z.rl), BF),
        V((nc, z.r1, cc), BF), V((nc, z.r1, cc), BF),
        V((z.pairs, z.rl), BF), V((z.pairs, z.rl), BF),
        V((nc, z.pairs, cc), BF), V((nc, z.pairs, cc), BF),
        V((8, 128), BF), V((nc, z.pairs, cc), BF),
        V((z.pairs, z.ff), F32), V((z.pairs, z.ff), F32), V((z.pairs, z.ff), F32),
        V((z.pairs, 2 * z.ff), BF), V((z.pairs, z.ff), BF), V((z.pairs, 128), F32),
        V((z.pairs, 128), F32), V((z.pairs, 128), F32),
        V((h, z.pairs, cc), BF), V((h, z.pairs, cc), BF), V((h, z.pairs, cc), BF),
        V((z.pairs, z.rl), BF), V((z.pairs, z.rl), BF),
        V((h, z.pairs, cc), BF), V((h, z.pairs, cc), BF),
        V((z.r1, z.rl), BF), V((z.r1, z.rl), BF),
        V((h, z.r1, cc), BF), V((h, z.r1, cc), BF),
        V((2, z.width), F32), V((2, z.width), F32),
        V((z.n_ep, z.rw, chd), F32), V((z.n_ep // 2, z.rw, chd), F32),
        V((z.rw, chd), F32), V((z.rw, chd), F32),
    ]
    D = pltpu.SemaphoreType.DMA
    sems = [
        D((nc + 2, z.groups)), D((nc + 2, z.groups)), D((nc + 1, z.gs)), D((nc + 1, z.gs)),
        D((nc, z.gs)), D((nc, z.gs)), D((h,)), D((h,)),
        D((h + 1, z.gs)), D((h + 1, z.gs)), D((h + 1, z.groups)), D((h + 1, z.groups)),
        D((3,)), D((3,)), D((z.n_ep // 2,)), D((z.n_ep // 2,)),
    ]
    spec = pl.BlockSpec(memory_space=pltpu.VMEM)
    tg, gate, up, down, gsq, usq, dsq, rout = pl.pallas_call(
        functools.partial(kernel, z),
        out_shape=[jax.ShapeDtypeStruct(s, d) for s, d in outs],
        in_specs=[spec] * 8,
        out_specs=[spec] * len(outs),
        scratch_shapes=scratch + sems,
        compiler_params=pltpu.CompilerParams(
            collective_id=0, has_side_effects=True, vmem_limit_bytes=44 * 2**20
        ),
    )(tokens, cotangent, routes.T, router_expert.T, router_group.T, gate_proj[0], up_proj[0], down_proj[0])
    if z.reduce_here:
        half = z.ch // 2
        shapes = [gate, up, down, tg, gsq, usq, dsq]
        anywhere = pl.BlockSpec(memory_space=pl.ANY)
        gate, up, down, tg, gsq, usq, dsq, reg, rgg, rrows = pl.pallas_call(
            functools.partial(finish, z),
            out_shape=[jax.ShapeDtypeStruct(a.shape, a.dtype) for a in shapes]
            + [jax.ShapeDtypeStruct((n, half), F32) for n in (z.experts, z.groups, 1)],
            in_specs=[spec] * 8,
            out_specs=[anywhere] * 7 + [spec] * 3,
            scratch_shapes=[D((7,))],
            compiler_params=pltpu.CompilerParams(vmem_limit_bytes=16 * 2**20),
        )(*shapes, rout)
        reg, rgg, rrows = reg.T, rgg.T, rrows[0]
    else:
        mine = lax.psum_scatter(rout.T, ("ep", "tp"), scatter_dimension=0, tiled=True)
        reg = mine[:, : z.experts]
        rgg = mine[:, z.experts : z.experts + z.groups]
        rrows = jnp.sum(reg * reg, axis=1) + jnp.sum(rgg * rgg, axis=1)
    return (tg, gate[None], up[None], down[None], gsq, usq, dsq, reg, rgg, rrows)


def solution(mesh):
    return jax.shard_map(
        functools.partial(body, dict(mesh.shape)),
        mesh=mesh,
        in_specs=(
            P("ep", None), P("ep", None), P("ep", None), P(), P(),
            P("ep", None, "tp"), P("ep", None, "tp"), P("ep", "tp", None),
        ),
        out_specs=(
            P("ep", "tp"), P("ep", None, "tp"), P("ep", None, "tp"), P("ep", "tp", None),
            P("ep", None), P("ep", None), P("ep", "tp"),
            P(("ep", "tp"), None), P(("ep", "tp"), None), P(("ep", "tp")),
        ),
        check_vma=False,
    )
```
